32 devices in a mesh: ra: 4 (over z), cb: 4 (over y, x), dp: 2 (over core).
Axes of the slice: x: 2, y: 2, z: 4, core: 2. Of those that a mesh axis runs over, the one named last changes fastest.
Arguments:
- tokens: bfloat16 [128, 4096], P('dp', 'ra'), may hold values from -45 to 45
- gain_first: bfloat16 [4096], P('ra'), may hold values from 0.099609375 to 1.8984375
- up_first: float32 [4096, 16384], P('ra', 'cb'), may hold values from -0.125 to 0.125
- up_scale_first: float32 [16384], P('cb'), may hold values from 0.5 to 2
- down_first: float32 [16384, 4096], P('cb', 'ra'), may hold values from -0.046875 to 0.046875
- down_scale_first: float32 [4096], P('ra'), may hold values from 0.5 to 2
- gain_second: bfloat16 [4096], P('ra'), may hold values from 0.099609375 to 1.8984375
- up_second: float32 [4096, 16384], P('ra', 'cb'), may hold values from -0.125 to 0.125
- up_scale_second: float32 [16384], P('cb'), may hold values from 0.5 to 2
- down_second: float32 [16384, 4096], P('cb', 'ra'), may hold values from -0.046875 to 0.046875
- down_scale_second: float32 [4096], P('ra'), may hold values from 0.5 to 2
Outputs:
- mixed_out: bfloat16 [128, 4096], P('dp', 'ra')
The draws below stay inside these ranges and needn't reach their ends.
All inputs are finite; a program needn't handle non-finite values.
Results may differ from the reference program's by a relative error of at most 0.02.
Values may be sent and summed in bfloat16 or wider, within the bound.
No kernel may reach another device: no remote copies, remote signals or barrier semaphores. Data moves between devices by JAX's collectives and lax.ppermute only.
A program may use at most 128 MiB of HBM per device.

```python
import math
import jax
import jax.numpy as jnp
from jax import lax

D = 4096
FF = 16384
TOKENS = 128
N_CB = 4


def draw_tokens(key, part):
    key_base = jax.random.fold_in(key, 11)
    key_cols = jax.random.fold_in(key, 12)
    key_rows = jax.random.fold_in(key, 13)
    columns = jnp.arange(D, dtype=jnp.float32) / D
    jitter = jax.random.uniform(key_cols, (D,), jnp.float32, -0.35, 0.35)
    col_scale = jnp.exp(math.log(10.0) * (columns - 0.5) + jitter)
    base = jnp.clip(jax.random.normal(key_base, (TOKENS, D), jnp.float32), -4.0, 4.0)
    row_scale = jnp.exp(jax.random.uniform(key_rows, (TOKENS, 1), jnp.float32, math.log(0.4), math.log(2.5)))
    return (base * row_scale * col_scale[None, :]).astype(jnp.bfloat16)


def strengthened(drawn, own_key, source, target, shards_of, factor):
    owner, partner = [(jnp.arange(drawn.shape[position]) // (drawn.shape[position] // shards_of)).reshape([-1 if axis == position else 1 for axis in range(drawn.ndim)]) for position in (source, target)]
    chosen = jax.random.permutation(own_key, shards_of)[partner]
    strong = (owner == chosen) | (owner == (partner + shards_of // 2) % shards_of)
    return jnp.where(strong, factor * drawn, drawn)


def steps_of(stream_key, extent, cuts, smallest, high):
    def one(dim, shards_of):
        heights = jax.random.uniform(jax.random.fold_in(jax.random.fold_in(stream_key, 6), dim), (shards_of,), jnp.float32, smallest / len(cuts), high / len(cuts))
        return jnp.repeat(jnp.exp(heights), extent[dim] // shards_of).reshape((-1,) + (1,) * (len(extent) - dim - 1))

    loudness = one(*cuts[0])
    for cut in cuts[1:]:
        loudness = loudness * one(*cut)
    return loudness


def bell_draw(key, shape, width, reach, split=(), kind=jnp.bfloat16):
    result = jax.random.normal(key, shape, jnp.float32) * width
    if len(split) > 0:
        result = steps_of(key, shape, split, -0.22, 0.18) * result
    return jnp.clip(result, min=-reach, max=reach).astype(kind)


def gaussian_with(own_key, dims, deviation, most, pieces, heavy, held_as=jnp.bfloat16):
    drawn = deviation * jax.random.normal(own_key, dims, jnp.float32)
    if pieces:
        drawn = drawn * steps_of(own_key, dims, pieces, -0.22, 0.18)
    return jnp.clip(strengthened(drawn, jax.random.fold_in(own_key, 3), *heavy), -most, most).astype(held_as)


def setup_inputs(seed: int = 0) -> dict:
    seeds = jax.random.split(jax.random.key(seed), 12)
    return {
        "tokens": draw_tokens(jax.random.fold_in(seeds[11], 71), 0),
        "gain_first": jnp.clip(1.0 + 0.18 * jax.random.normal(seeds[1], (D,), jnp.float32), 0.099609375, 1.8984375).astype(jnp.bfloat16),
        "up_first": gaussian_with(seeds[2], (D, FF), D ** -0.5, 0.125, ((0, 4), (1, 4)), (0, 1, 4, 2.0), jnp.float32),
        "up_scale_first": jnp.clip(jnp.exp(math.log(2.0) - 1.3862944 * jax.random.uniform(seeds[3], (FF,), jnp.float32) ** steps_of(seeds[3], (FF,), ((0, 4),), -0.2, 0.2)), 0.5, 2.0),
        "down_first": bell_draw(seeds[4], (FF, D), FF ** -0.5, 0.046875, ((0, 4), (1, 4)), jnp.float32),
        "down_scale_first": jnp.clip(jnp.exp(math.log(2.0) - 1.3862944 * jax.random.uniform(seeds[5], (D,), jnp.float32) ** steps_of(seeds[5], (D,), ((0, 4),), -0.2, 0.2)), 0.5, 2.0),
        "gain_second": jnp.clip(1.0 + 0.18 * jax.random.normal(seeds[6], (D,), jnp.float32), 0.099609375, 1.8984375).astype(jnp.bfloat16),
        "up_second": gaussian_with(seeds[7], (D, FF), D ** -0.5, 0.125, ((0, 4), (1, 4)), (0, 1, 4, 2.0), jnp.float32),
        "up_scale_second": jnp.clip(jnp.exp(math.log(2.0) - 1.3862944 * jax.random.uniform(seeds[8], (FF,), jnp.float32) ** steps_of(seeds[8], (FF,), ((0, 4),), -0.2, 0.2)), 0.5, 2.0),
        "down_second": bell_draw(seeds[9], (FF, D), FF ** -0.5, 0.046875, ((0, 4), (1, 4)), jnp.float32),
        "down_scale_second": jnp.clip(jnp.exp(math.log(2.0) - 1.3862944 * jax.random.uniform(seeds[10], (D,), jnp.float32) ** steps_of(seeds[10], (D,), ((0, 4),), -0.2, 0.2)), 0.5, 2.0),
    }


epsilon = 1e-06
residual_share = 0.25

def sub_layer(inputs, norm_gain, up_weight, up_scale, down_weight, down_scale):
    values = inputs.astype(jnp.float32)
    mean_square = lax.optimization_barrier(jnp.mean(values * values, axis=-1, keepdims=True))
    normed = (values * lax.rsqrt(mean_square + epsilon) * norm_gain.astype(jnp.float32)).astype(jnp.bfloat16)
    upward = jnp.dot(normed, up_weight.astype(jnp.bfloat16), preferred_element_type=jnp.float32) * up_scale
    hidden = jnp.square(jax.nn.relu(upward)).astype(jnp.bfloat16)
    down_bf = down_weight.astype(jnp.bfloat16)
    block_rows = hidden.shape[1] // N_CB
    total = jnp.zeros((inputs.shape[0], down_weight.shape[1]), jnp.float32)
    for block in range(N_CB):
        lower = block * block_rows
        part = jnp.dot(hidden[:, lower:lower + block_rows], down_bf[lower:lower + block_rows, :], preferred_element_type=jnp.float32).astype(jnp.bfloat16)
        total = total + lax.optimization_barrier(part).astype(jnp.float32)
    return (residual_share * values + total * down_scale).astype(jnp.bfloat16)

def reference(tokens, gain_first, up_first, up_scale_first, down_first, down_scale_first, gain_second, up_second, up_scale_second, down_second, down_scale_second):
    carried = sub_layer(tokens, gain_first, up_first, up_scale_first, down_first, down_scale_first)
    return sub_layer(carried, gain_second, up_second, up_scale_second, down_second, down_scale_second)
```

```python
import jax
import jax.numpy as jnp
from jax import lax
from jax.sharding import PartitionSpec as P

epsilon = 1e-06
residual_share = 0.25


def shifted(value, axis, step):
    size = lax.axis_size(axis)
    return lax.ppermute(value, axis, [(i, (i + step) % size) for i in range(size)])


def gathered_sum(value, axis):
    total = value.astype(jnp.float32)
    for step in range(1, lax.axis_size(axis)):
        total = total + shifted(value, axis, step).astype(jnp.float32)
    return total


def sub_layer(inputs, norm_gain, up_weight, up_scale, down_weight, down_scale):
    values = inputs.astype(jnp.float32)
    ra = lax.axis_size("ra")
    own = lax.axis_index("ra")
    full_width = inputs.shape[1] * ra
    squares = gathered_sum(jnp.sum(values * values, axis=1)[None, :], "ra")
    inverse = lax.rsqrt(squares / full_width + epsilon)[0][:, None]
    gained = (values * norm_gain.astype(jnp.float32)).astype(jnp.bfloat16)
    width = up_weight.shape[1] // ra

    def up_part(step):
        first = ((own + step) % ra) * width
        block = lax.dynamic_slice_in_dim(up_weight, first, width, 1)
        return jnp.dot(gained, block.astype(jnp.bfloat16), preferred_element_type=jnp.float32)

    arrived = [
        shifted(up_part(step).astype(jnp.bfloat16), "ra", step) for step in range(1, ra)
    ]
    upward = up_part(0)
    for other in arrived:
        upward = upward + other.astype(jnp.float32)
    own_scale = lax.dynamic_slice_in_dim(up_scale, own * width, width, 0)
    units = jnp.square(jax.nn.relu(upward * inverse * own_scale)).astype(jnp.bfloat16)

    def down_part(block, step):
        first = ((own - step) % ra) * width
        rows = lax.dynamic_slice_in_dim(down_weight, first, width, 0)
        return jnp.dot(block, rows.astype(jnp.bfloat16), preferred_element_type=jnp.float32)

    others = [shifted(units, "ra", step) for step in range(1, ra)]
    projected = down_part(units, 0)
    for step in range(1, ra):
        projected = projected + down_part(others[step - 1], step)
    total = gathered_sum(projected.astype(jnp.bfloat16), "cb")
    return (residual_share * values + total * down_scale).astype(jnp.bfloat16)


def shards(
    tokens,
    gain_first,
    up_first,
    up_scale_first,
    down_first,
    down_scale_first,
    gain_second,
    up_second,
    up_scale_second,
    down_second,
    down_scale_second,
):
    carried = sub_layer(tokens, gain_first, up_first, up_scale_first, down_first, down_scale_first)
    return sub_layer(
        carried, gain_second, up_second, up_scale_second, down_second, down_scale_second
    )


def solution(mesh):
    in_specs = (
        P("dp", "ra"),
        P("ra"),
        P("ra", "cb"),
        P("cb"),
        P("cb", "ra"),
        P("ra"),
        P("ra"),
        P("ra", "cb"),
        P("cb"),
        P("cb", "ra"),
        P("ra"),
    )
    out_specs = P("dp", "ra")
    return jax.shard_map(shards, mesh=mesh, in_specs=in_specs, out_specs=out_specs, check_vma=False)
```

```python
import jax
import jax.numpy as jnp
from jax import lax
from jax.sharding import PartitionSpec as P

epsilon = 1e-06
residual_share = 0.25


def shifted(value, axis, step):
    size = lax.axis_size(axis)
    return lax.ppermute(value, axis, [(i, (i + step) % size) for i in range(size)])


def gathered_sum(value, axis):
    total = value.astype(jnp.float32)
    for step in range(1, lax.axis_size(axis)):
        total = total + shifted(value, axis, step).astype(jnp.float32)
    return total


lanes = 128


def sent_order(size):
    return sorted(range(1, size), key=lambda step: (-min(step, size - step), step))


def sub_layer(inputs, norm_gain, up_weight, up_scale, down_weight, down_scale):
    values = inputs.astype(jnp.float32)
    ra = lax.axis_size("ra")
    own = lax.axis_index("ra")
    full_width = inputs.shape[1] * ra
    squares = jnp.sum(values * values, axis=1, keepdims=True)
    gained = (values * norm_gain.astype(jnp.float32)).astype(jnp.bfloat16)
    width = up_weight.shape[1] // ra

    def up_part(step):
        first = ((own + step) % ra) * width
        block = (lax.dynamic_slice_in_dim(up_weight, first, width, 1))
        return jnp.dot(gained, block.astype(jnp.bfloat16), preferred_element_type=jnp.float32)

    sends = sent_order(ra)
    arrived = []
    for place, step in enumerate(sends):
        part = up_part(step).astype(jnp.bfloat16)
        arrived.append(shifted(part, "ra", step))
    upward = lax.optimization_barrier(up_part(0))
    for other in arrived:
        upward = upward + other.astype(jnp.float32)
    own_scale = lax.dynamic_slice_in_dim(up_scale, own * width, width, 0)
    units = jnp.square(jax.nn.relu(upward * own_scale)).astype(jnp.bfloat16)

    high = lax.reduce_precision(squares, 8, 7)
    lane = lax.broadcasted_iota(jnp.int32, (inputs.shape[0], lanes), 1)
    tail = jnp.where(lane == 0, high, jnp.where(lane == 1, squares - high, 0.0))
    message = jnp.concatenate([units, tail.astype(jnp.bfloat16)], axis=1)

    def down_part(block, mask):
        rows = lax.dynamic_slice_in_dim(down_weight, (own ^ mask) * width, width, 0)
        return jnp.dot(block, rows.astype(jnp.bfloat16), preferred_element_type=jnp.float32)

    held = {0: message}
    bit = ra // 2
    place = 0
    while bit:
        for mask in list(held):
            held[mask | bit] = lax.ppermute(
                held[mask], "ra", [(i, i ^ bit) for i in range(ra)]
            )
            place += 1
        bit //= 2
    projected = down_part(units, 0)
    near_first = sorted(list(held)[1:], key=lambda mask: (mask.bit_count(), mask))
    for place, mask in enumerate(near_first):
        projected = projected + down_part(held[mask][:, :width], mask)
        tail = held[mask][:, width:].astype(jnp.float32)
        squares = squares + jnp.sum(tail, axis=1, keepdims=True)
    part = projected / (squares / full_width + epsilon)
    total = gathered_sum(part.astype(jnp.bfloat16), "cb")
    return (residual_share * values + total * down_scale).astype(jnp.bfloat16)


def shards(
    tokens,
    gain_first,
    up_first,
    up_scale_first,
    down_first,
    down_scale_first,
    gain_second,
    up_second,
    up_scale_second,
    down_second,
    down_scale_second,
):
    carried = sub_layer(tokens, gain_first, up_first, up_scale_first, down_first, down_scale_first)
    return sub_layer(
        carried, gain_second, up_second, up_scale_second, down_second, down_scale_second
    )


def solution(mesh):
    in_specs = (
        P("dp", "ra"),
        P("ra"),
        P("ra", "cb"),
        P("cb"),
        P("cb", "ra"),
        P("ra"),
        P("ra"),
        P("ra", "cb"),
        P("cb"),
        P("cb", "ra"),
        P("ra"),
    )
    out_specs = P("dp", "ra")
    return jax.shard_map(shards, mesh=mesh, in_specs=in_specs, out_specs=out_specs, check_vma=False)
```
